32 devices in a mesh: grp: 2 (over y), sp: 4 (over z), tp: 4 (over x, core).
Axes of the slice: x: 2, y: 2, z: 4, core: 2. Of those that a mesh axis runs over, the one named last changes fastest.
Arguments:
- tokens: bfloat16 [8, 1024, 4096], P(('grp', 'tp'), 'sp'), parts along dimension 0, may hold values from -8 to 8, as said below
- offsets: int32 [8], P(('grp', 'tp')), parts along dimension 0, may hold values from 0 to 4095
- in_gain: float32 [4096], replicated, may hold values from 0.1 to 1.9
- w_latent: bfloat16 [4096, 1024], P('sp'), may hold values from -0.09375 to 0.09375
- w_rope_key: bfloat16 [4096, 32], replicated, may hold values from -0.09375 to 0.09375
- kv_gain: float32 [1024], replicated, may hold values from 0.1 to 1.9
- w_up_key: bfloat16 [1024, 2048], P(None, 'tp'), may hold values from -0.1875 to 0.1875
- w_up_value: bfloat16 [1024, 2048], P(None, 'tp'), may hold values from -0.1875 to 0.1875
- q_nope: bfloat16 [8, 2048], P(('grp', 'sp'), 'tp'), parts along dimension 0, may hold values from -300 to 300, as said below
- q_rope: bfloat16 [8, 1024], P(('grp', 'sp'), 'tp'), parts along dimension 0, may hold values from -16 to 16
Outputs:
- keys: bfloat16 [8, 1024, 2048], P(('grp', 'sp'), None, 'tp'), parts along dimension 0
- values: bfloat16 [8, 1024, 2048], P(('grp', 'sp'), None, 'tp'), parts along dimension 0
- rope_keys: bfloat16 [8, 32, 1024], P(('grp', 'sp')), parts along dimension 0
- read: bfloat16 [8, 2048], P(('grp', 'sp'), 'tp'), parts along dimension 0
The draws below stay inside these ranges and needn't reach their ends.
There are 2 independent parts, one for each index of `grp`. The reference program is written for one: setup_inputs(seed, part) draws one part's arguments, and reference() takes and returns one part's arrays. A program takes and returns all parts, laid end to end along the dimension named above; an argument that names none is the same for every part. Nothing has to cross between parts.
Inputs may be any that keep to these rules, and one draw needn't show every extreme that they name: `tokens`: entries of the layer's input. `q_nope`: entries of the first decoding token's queries.
All inputs are finite; a program needn't handle non-finite values.
Results may differ from the reference program's by a relative error of at most 0.02.
Values may be sent and summed in bfloat16 or wider, within the bound.
No kernel may reach another device: no remote copies, remote signals or barrier semaphores. Data moves between devices by JAX's collectives and lax.ppermute only.
A program may use at most 128 MiB of HBM per device.

```python
import jax
import jax.numpy as jnp
from jax import lax

D = 4096
HEADS = 32
HEAD = 64
ROPE = 32
KV_RANK = 1024
SEQS = 4
LEN = 1024


def draw_tokens(key, part):
    first, second = jax.random.split(jax.random.fold_in(key, 29))
    noise = jax.random.normal(first, (SEQS, LEN, D), jnp.float32)
    base = jnp.clip(noise, -6.0, 6.0)
    return base.astype(jnp.bfloat16)


def draw_q_nope(key, part):
    first, second = jax.random.split(jax.random.fold_in(key, 17))
    base = jax.random.normal(first, (SEQS, HEADS, HEAD), jnp.float32) * 4.0
    base = jnp.clip(base, -16.0, 16.0)
    return base.reshape(SEQS, HEADS * HEAD).astype(jnp.bfloat16)


def plant(array, key, low, largest):
    place = [jax.random.randint(jax.random.fold_in(key, axis), (), 0, length) for axis, length in enumerate(array.shape)]
    widest = array.shape.index(max(array.shape))
    neighbour = place[:widest] + [(place[widest] + 1) % array.shape[widest]] + place[widest + 1:]
    return array.at[tuple(place)].set(low).at[tuple(neighbour)].set(largest)


def block_levels(stream_key, extent, pieces, low, top_value):
    loudness = 1.0
    for dim, parts in pieces:
        steps = jax.random.uniform(jax.random.fold_in(jax.random.fold_in(stream_key, 6), dim), (parts,), jnp.float32, low / len(pieces), top_value / len(pieces))
        loudness = loudness * jnp.repeat(jnp.exp(steps), extent[dim] // parts).reshape((-1,) + (1,) * (len(extent) - 1 - dim))
    return loudness


def normal_values(key, extent, deviation, reach, shards=(), kind=jnp.bfloat16):
    drawn = deviation * jax.random.normal(key, extent, jnp.float32)
    if shards:
        drawn = drawn * block_levels(key, extent, shards, -0.22, 0.18)
    return jnp.clip(drawn, -reach, reach).astype(kind)


def setup_inputs(seed: int = 0, part: int = 0) -> dict:
    key_list = jax.random.split(jax.random.key(seed), 11)
    own_keys = jax.random.split(jax.random.fold_in(key_list[10], part), 11)
    return {
        "tokens": draw_tokens(jax.random.fold_in(jax.random.fold_in(key_list[10], part), 71), part),
        "offsets": plant(jax.random.randint(own_keys[1], (SEQS,), 0, 4096), jax.random.fold_in(own_keys[1], 1), 0, 4095).astype(jnp.int32),
        "in_gain": jnp.clip(1.0 + 0.18 * jax.random.normal(key_list[2], (D,), jnp.float32), 0.1, 1.9),
        "w_latent": normal_values(key_list[3], (D, KV_RANK), D ** -0.5, 0.09375, ((0, 4),)),
        "w_rope_key": normal_values(key_list[4], (D, ROPE), D ** -0.5, 0.09375),
        "kv_gain": jnp.clip(1.0 + 0.18 * jax.random.normal(key_list[5], (KV_RANK,), jnp.float32), 0.1, 1.9),
        "w_up_key": normal_values(key_list[6], (KV_RANK, HEADS * HEAD), KV_RANK ** -0.5, 0.1875, ((1, 4),)),
        "w_up_value": normal_values(key_list[7], (KV_RANK, HEADS * HEAD), KV_RANK ** -0.5, 0.1875, ((1, 4),)),
        "q_nope": draw_q_nope(jax.random.fold_in(jax.random.fold_in(key_list[10], part), 71), part),
        "q_rope": normal_values(own_keys[9], (SEQS, HEADS * ROPE), 4.0, 16.0, ((0, 4), (1, 4))),
    }


EPS = 1e-06

def rms_scale(values, gain):
    wide = values.astype(jnp.float32)
    return wide * lax.rsqrt(lax.optimization_barrier(jnp.mean(wide * wide, axis=-1, keepdims=True)) + EPS) * gain.astype(jnp.float32)

def rotate(raw, position):
    inverse = 10000.0 ** (-jnp.arange(0, ROPE, 2).astype(jnp.float32) / ROPE)
    angle = position.astype(jnp.float32)[:, None] * inverse[None, :]
    cosine, sine = (jnp.cos(angle), jnp.sin(angle))
    half = ROPE // 2
    first, second = (raw[:, :half], raw[:, half:])
    return jnp.concatenate([first * cosine - second * sine, second * cosine + first * sine], axis=-1)

def reference(tokens, offsets, in_gain, w_latent, w_rope_key, kv_gain, w_up_key, w_up_value, q_nope, q_rope):

    def one_prompt(args):
        prompt, start = args
        normed = rms_scale(prompt, in_gain).astype(jnp.bfloat16)
        latent_raw = jnp.dot(normed, w_latent, preferred_element_type=jnp.float32)
        latent = rms_scale(latent_raw, kv_gain).astype(jnp.bfloat16)
        rope_raw = jnp.dot(normed, w_rope_key, preferred_element_type=jnp.float32)
        position = start + jnp.arange(LEN, dtype=jnp.int32)
        rotated = rotate(rope_raw, position).astype(jnp.bfloat16)
        keys = jnp.dot(latent, w_up_key, preferred_element_type=jnp.float32).astype(jnp.bfloat16)
        values = jnp.dot(latent, w_up_value, preferred_element_type=jnp.float32).astype(jnp.bfloat16)
        return (keys, values, rotated.T)
    keys, values, rope_keys = lax.map(one_prompt, (tokens, offsets))
    query = q_nope.astype(jnp.float32).reshape(SEQS, HEADS, HEAD)
    rotary_q = q_rope.astype(jnp.float32).reshape(SEQS, HEADS, ROPE)
    keys_wide = keys.astype(jnp.float32).reshape(SEQS, LEN, HEADS, HEAD)
    scores = jnp.einsum('shd,sjhd->shj', query, keys_wide)
    scores = scores + jnp.einsum('shr,srj->shj', rotary_q, rope_keys.astype(jnp.float32))
    scores = scores / jnp.sqrt(jnp.float32(HEAD + ROPE))
    weights = jax.nn.softmax(scores, axis=-1).astype(jnp.bfloat16)
    values_wide = values.astype(jnp.float32).reshape(SEQS, LEN, HEADS, HEAD)
    read = jnp.einsum('shj,sjhd->shd', weights.astype(jnp.float32), values_wide)
    read = read.astype(jnp.bfloat16).reshape(SEQS, HEADS * HEAD)
    return (keys, values, rope_keys, read)
```

```python
import jax
import jax.numpy as jnp
from jax import lax
from jax.sharding import PartitionSpec as P

HEAD = 64
ROPE = 32


EPS = 1e-06


def rms_scale(values, gain):
    wide = values.astype(jnp.float32)
    return wide * lax.rsqrt(jnp.mean(wide * wide, axis=-1, keepdims=True) + EPS) * gain


def rotate(raw, position):
    inverse = 10000.0 ** (-jnp.arange(0, ROPE, 2).astype(jnp.float32) / ROPE)
    angle = position.astype(jnp.float32)[..., None] * inverse
    cosine, sine = (jnp.cos(angle), jnp.sin(angle))
    half = ROPE // 2
    first, second = (raw[..., :half], raw[..., half:])
    return jnp.concatenate(
        [first * cosine - second * sine, second * cosine + first * sine], axis=-1
    )


def attend(keys, values, rope_keys, q_nope, q_rope):
    length, head_cols = keys.shape
    heads_here = head_cols // HEAD
    query = q_nope.reshape(heads_here, HEAD)
    rotary_q = q_rope.reshape(heads_here, ROPE)
    keys_split = keys.reshape(length, heads_here, HEAD)
    scores = jnp.einsum("hd,jhd->hj", query, keys_split, preferred_element_type=jnp.float32)
    scores = scores + jnp.dot(rotary_q, rope_keys, preferred_element_type=jnp.float32)
    scores = scores / jnp.sqrt(jnp.float32(HEAD + ROPE))
    peak = jnp.max(scores, axis=-1, keepdims=True)
    expo = jnp.exp(scores - peak)
    weights = (expo / jnp.sum(expo, axis=-1, keepdims=True)).astype(jnp.bfloat16)
    read = jnp.einsum(
        "hj,jhd->hd",
        weights,
        values.reshape(length, heads_here, HEAD),
        preferred_element_type=jnp.float32,
    )
    return read.astype(jnp.bfloat16).reshape(1, heads_here * HEAD)


def swap(value, axis, bits):
    n = lax.axis_size(axis)
    return lax.ppermute(value, axis, [(i, i ^ bits) for i in range(n)])


def ordered(blocks, index, total):
    stacked = jnp.concatenate([block[None] for block in blocks], axis=0)
    return jnp.concatenate(
        [lax.dynamic_index_in_dim(stacked, n ^ index, 0, keepdims=True) for n in range(total)], axis=0
    )


def spread(
    tokens, offsets, in_gain, w_latent, w_rope_key, kv_gain, w_up_key, w_up_value, q_nope, q_rope
):
    prompts, rows, width = tokens.shape
    n_sp, n_tp, n_grp = (lax.axis_size("sp"), lax.axis_size("tp"), lax.axis_size("grp"))
    n_x = n_tp // 2
    z, t, y = (lax.axis_index("sp"), lax.axis_index("tp"), lax.axis_index("grp"))
    x, c = (t // 2, t % 2)
    rank = w_latent.shape[1]
    half = rank // 2
    k_block = w_latent.shape[0]
    piece = k_block // (n_x * n_grp)

    mine = lax.dynamic_slice(w_latent, ((x * n_grp + y) * piece, c * half), (piece, half))
    far = {}
    for i in range(1, n_sp):
        far[i] = swap(mine, "sp", i)
    pieces = {}
    for i in range(1, n_sp):
        held = {(0, 0): far[i]}
        for j in range(1, n_x):
            held[j, 0] = swap(far[i], "tp", 2 * j)
        for j in range(n_x):
            for g in range(1, n_grp):
                held[j, g] = swap(held[j, 0], "grp", g)
        pieces[i] = held

    normed = rms_scale(tokens.reshape(prompts * rows, width), in_gain).astype(jnp.bfloat16)
    position = offsets[:, None] + z * rows + jnp.arange(rows, dtype=jnp.int32)[None, :]
    rope_raw = jnp.dot(normed, w_rope_key, preferred_element_type=jnp.float32).reshape(
        prompts, rows, ROPE
    )
    rotated = rotate(rope_raw, position).astype(jnp.bfloat16)
    came = []
    for r in range(prompts):
        turn = lambda s: (r + s) % prompts
        send = lax.dynamic_index_in_dim(rotated, turn(z), 0, keepdims=False)
        came.append(
            lax.ppermute(
                send,
                ("sp", "tp"),
                [
                    (s * n_tp + u, (prompts * u + turn(s)) * n_tp + s // prompts)
                    for s in range(n_sp)
                    for u in range(n_tp)
                ],
            )
        )
    came = jnp.stack(came)
    if prompts > 1:
        came = jnp.concatenate(
            [
                lax.dynamic_index_in_dim(came, (z - s) % prompts, 0, keepdims=True)
                for s in range(prompts)
            ],
            axis=0,
        )
    ropes = [came]
    for b in range(n_tp.bit_length() - 1):
        ropes = ropes + [swap(block, "tp", 1 << b) for block in ropes]
    rope_keys = ordered(ropes, t, n_tp).reshape(n_sp * rows, ROPE).T

    parts = []
    for i in range(n_sp):
        block = lax.dynamic_slice(normed, (0, (z ^ i) * k_block), (prompts * rows, k_block))
        if i:
            block = jnp.concatenate(
                [
                    lax.dynamic_slice(
                        block,
                        (0, ((x ^ j) * n_grp + (y ^ g)) * piece),
                        (prompts * rows, piece),
                    )
                    for j in range(n_x)
                    for g in range(n_grp)
                ],
                axis=1,
            )
        parts.append(block)
    mine_rows = jnp.concatenate(parts, axis=1)
    both_rows = jnp.concatenate([mine_rows, swap(mine_rows, "tp", 1)], axis=0)
    raw = jnp.dot(
        both_rows[:, :k_block],
        lax.dynamic_slice(w_latent, (0, c * half), (k_block, half)),
        preferred_element_type=jnp.float32,
    )
    for i in range(1, n_sp):
        weight = jnp.concatenate(
            [pieces[i][j, g] for j in range(n_x) for g in range(n_grp)], axis=0
        )
        raw = raw + jnp.dot(
            both_rows[:, i * k_block : (i + 1) * k_block],
            weight,
            preferred_element_type=jnp.float32,
        )
    squares = jnp.sum(raw * raw, axis=1)
    other = swap(squares, "tp", 1)
    own = prompts * rows
    mean = (squares + jnp.concatenate([other[own:], other[:own]])) / rank
    gain_here = lax.dynamic_slice(kv_gain, (c * half,), (half,))
    latent = (raw * lax.rsqrt(mean + EPS)[:, None] * gain_here).astype(jnp.bfloat16)

    per_chip = 2 * prompts
    sub = rows // n_x
    latent = latent.reshape(2, prompts, n_x, sub, half)
    latent = jnp.concatenate(
        [lax.dynamic_index_in_dim(latent, k ^ c, 0, keepdims=True) for k in range(2)], axis=0
    ).reshape(per_chip, n_x, sub, half)
    over_x = [lax.dynamic_index_in_dim(latent, x, 1, keepdims=False)]
    for j in range(1, n_x):
        over_x.append(
            swap(lax.dynamic_index_in_dim(latent, x ^ j, 1, keepdims=False), "tp", 2 * j)
        )
    prompts_here = jnp.stack(over_x).reshape(n_x * per_chip, sub, half)
    blocks = []
    for i in range(n_sp):
        p = z ^ i
        block = lax.dynamic_index_in_dim(
            prompts_here, ((p // per_chip) ^ x) * per_chip + p % per_chip, 0, keepdims=False
        )
        blocks.append(swap(block, "sp", i) if i else block)
    column = ordered(blocks, z, n_sp)
    columns = [column]
    for j in range(1, n_x):
        columns.append(swap(column, "tp", 2 * j))
    here = ordered(columns, x, n_x).transpose(1, 0, 2, 3).reshape(n_sp * rows, half)
    there = swap(here, "tp", 1)

    def up(weight):
        first = lax.dynamic_slice(weight, (c * half, 0), (half, weight.shape[1]))
        second = lax.dynamic_slice(weight, ((1 - c) * half, 0), (half, weight.shape[1]))
        return (
            jnp.dot(here, first, preferred_element_type=jnp.float32)
            + jnp.dot(there, second, preferred_element_type=jnp.float32)
        ).astype(jnp.bfloat16)

    keys, values = (up(w_up_key), up(w_up_value))
    read = attend(keys, values, rope_keys, q_nope, q_rope)
    return (keys[None], values[None], rope_keys[None], read)


def gathered(
    tokens, offsets, in_gain, w_latent, w_rope_key, kv_gain, w_up_key, w_up_value, q_nope, q_rope
):
    prompts, rows, width = tokens.shape
    n_sp = lax.axis_size("sp")
    length = n_sp * rows
    block = lax.axis_index("sp")
    normed = rms_scale(tokens.reshape(prompts * rows, width), in_gain).astype(jnp.bfloat16)
    latent_raw = jnp.dot(
        normed,
        lax.all_gather(w_latent, "sp", axis=0, tiled=True),
        preferred_element_type=jnp.float32,
    )
    latent = rms_scale(latent_raw, kv_gain).astype(jnp.bfloat16)
    position = offsets[:, None] + block * rows + jnp.arange(rows, dtype=jnp.int32)[None, :]
    rope_raw = jnp.dot(normed, w_rope_key, preferred_element_type=jnp.float32).reshape(
        prompts, rows, ROPE
    )
    rotated = rotate(rope_raw, position).astype(jnp.bfloat16)
    latent_every, rope_every = (
        lax.all_gather(latent.reshape(prompts, rows, latent.shape[1]), "tp", axis=0, tiled=True),
        lax.all_gather(rotated, "tp", axis=0, tiled=True),
    )
    latent_moved, rope_moved = (
        lax.all_to_all(latent_every[:, None], "sp", split_axis=0, concat_axis=1, tiled=True),
        lax.all_to_all(rope_every[:, None], "sp", split_axis=0, concat_axis=1, tiled=True),
    )
    latent_all = latent_moved.reshape(length, latent_moved.shape[3])
    keys = jnp.dot(latent_all, w_up_key, preferred_element_type=jnp.float32).astype(jnp.bfloat16)
    values = jnp.dot(latent_all, w_up_value, preferred_element_type=jnp.float32).astype(
        jnp.bfloat16
    )
    rope_keys = rope_moved.reshape(length, ROPE).T
    read = attend(keys, values, rope_keys, q_nope, q_rope)
    return (keys[None], values[None], rope_keys[None], read)


def local(tokens, *rest):
    prompts, rows, _ = tokens.shape
    n_sp, n_tp, n_grp = (lax.axis_size("sp"), lax.axis_size("tp"), lax.axis_size("grp"))
    w_latent = rest[2]
    twos = all(n & (n - 1) == 0 for n in (n_sp, n_tp, n_grp))
    if (
        twos
        and n_tp > 1
        and n_sp == prompts * n_tp
        and rows % (n_tp // 2) == 0
        and w_latent.shape[0] % (n_tp // 2 * n_grp) == 0
        and w_latent.shape[1] % 2 == 0
    ):
        return spread(tokens, *rest)
    return gathered(tokens, *rest)


def solution(mesh):
    in_specs = (
        P(("grp", "tp"), "sp", None),
        P(("grp", "tp")),
        P(),
        P("sp", None),
        P(),
        P(),
        P(None, "tp"),
        P(None, "tp"),
        P(("grp", "sp"), "tp"),
        P(("grp", "sp"), "tp"),
    )
    out_specs = (
        P(("grp", "sp"), None, "tp"),
        P(("grp", "sp"), None, "tp"),
        P(("grp", "sp"), None, None),
        P(("grp", "sp"), "tp"),
    )
    return jax.shard_map(local, mesh=mesh, in_specs=in_specs, out_specs=out_specs, check_vma=False)
```

```python
import jax
import jax.numpy as jnp
import numpy as np
from jax import lax
from jax.experimental import pallas as pl
from jax.experimental.pallas import tpu as pltpu
from jax.sharding import PartitionSpec as P


HEAD = 64
ROPE = 32


EPS = 1e-06


def rms_scale(values, gain):
    wide = values.astype(jnp.float32)
    return wide * lax.rsqrt(jnp.mean(wide * wide, axis=-1, keepdims=True) + EPS) * gain


def rotate(raw, position):
    inverse = 10000.0 ** (-jnp.arange(0, ROPE, 2).astype(jnp.float32) / ROPE)
    angle = position.astype(jnp.float32)[..., None] * inverse
    cosine, sine = (jnp.cos(angle), jnp.sin(angle))
    half = ROPE // 2
    first, second = (raw[..., :half], raw[..., half:])
    return jnp.concatenate(
        [first * cosine - second * sine, second * cosine + first * sine], axis=-1
    )


def rotate_first(raw, position):
    inverse = 10000.0 ** (-jnp.arange(0, ROPE, 2).astype(jnp.float32) / ROPE)
    angle = position.astype(jnp.float32)[None] * inverse[:, None, None]
    cosine, sine = (jnp.cos(angle), jnp.sin(angle))
    half = ROPE // 2
    first, second = (raw[:half], raw[half:])
    return jnp.concatenate(
        [first * cosine - second * sine, second * cosine + first * sine], axis=0
    )


def attend(keys, values, rope_keys, q_nope, q_rope):
    length, head_cols = keys.shape
    heads_here = head_cols // HEAD
    query = q_nope.reshape(heads_here, HEAD)
    rotary_q = q_rope.reshape(heads_here, ROPE)
    keys_split = keys.reshape(length, heads_here, HEAD)
    scores = jnp.einsum("hd,jhd->hj", query, keys_split, preferred_element_type=jnp.float32)
    scores = scores + jnp.dot(rotary_q, rope_keys, preferred_element_type=jnp.float32)
    scores = scores / jnp.sqrt(jnp.float32(HEAD + ROPE))
    peak = jnp.max(scores, axis=-1, keepdims=True)
    expo = jnp.exp(scores - peak)
    weights = (expo / jnp.sum(expo, axis=-1, keepdims=True)).astype(jnp.bfloat16)
    read = jnp.einsum(
        "hj,jhd->hd",
        weights,
        values.reshape(length, heads_here, HEAD),
        preferred_element_type=jnp.float32,
    )
    return read.astype(jnp.bfloat16).reshape(1, heads_here * HEAD)


def swap(value, axis, bits):
    n = lax.axis_size(axis)
    return lax.ppermute(value, axis, [(i, i ^ bits) for i in range(n)])


class Table:
    def __init__(self, scalars):
        self.scalars = scalars
        self.rows = []
        self.more = []

    def add(self, more=0, **terms):
        self.rows.append(terms)
        self.more.append(more)
        return len(self.rows) - 1

    def build(self):
        total = jnp.asarray(np.array(self.more, np.int32))
        for name, scalar in self.scalars.items():
            number = np.array([row.get(name, (0, 0))[0] for row in self.rows], np.int32)
            factor = np.array([row.get(name, (0, 0))[1] for row in self.rows], np.int32)
            total = total + (scalar.astype(jnp.int32) ^ number) * factor
        return total


def spread(
    tokens, offsets, in_gain, w_latent, w_rope_key, kv_gain, w_up_key, w_up_value, q_nope, q_rope
):
    prompts, rows, width = tokens.shape
    n_sp, n_tp, n_grp = (lax.axis_size("sp"), lax.axis_size("tp"), lax.axis_size("grp"))
    n_x = n_tp // 2
    z, t, y = (lax.axis_index("sp"), lax.axis_index("tp"), lax.axis_index("grp"))
    x, c = (t // 2, t % 2)
    rank = w_latent.shape[1]
    half = rank // 2
    k_block = w_latent.shape[0]
    own = prompts * rows
    per_chip = 2 * prompts
    sub = rows // n_x

    piece = k_block // n_grp // n_x
    mine = []
    source = w_latent
    for a in range(n_x):
        mine.append(
            lax.dynamic_slice(source, ((y * n_x + (x ^ a)) * piece, c * half), (piece, half))
        )
        source, mine[a] = lax.optimization_barrier((source, mine[a]))
    base = {(i, a): swap(mine[a], "sp", i) for i, a in fetches(n_sp, n_x)}
    corner = (n_sp - 1, 0)
    weights = {}
    for i, a in base:
        for g in range(n_grp):
            weights[i, a, 0, g] = swap(base[i, a], "grp", g) if g else base[i, a]
            if (i, a) == corner:
                for j in range(1, n_x):
                    weights[i, a, j, g] = swap(weights[i, a, 0, g], "tp", 2 * j)

    normed = lax.optimization_barrier(
        rms_scale(tokens.reshape(own, width), in_gain).astype(jnp.bfloat16)
    )
    shares = normed.reshape(prompts, n_x, sub, width)
    came = {}
    for j in range(1, n_x):
        share = lax.dynamic_index_in_dim(shares, x ^ j, 1, keepdims=False).reshape(-1, width)
        came[j] = swap(share, "tp", 2 * j)
    taken = []
    for s in range(2):
        taken.append(swap(normed, "tp", 1) if s else normed)
        taken += [swap(came[j], "tp", 1) if s else came[j] for j in range(1, n_x)]

    position = offsets[:, None] + z * rows + jnp.arange(rows, dtype=jnp.int32)[None, :]
    rope_raw = lax.dot_general(
        w_rope_key, normed, (((0,), (1,)), ((), ())), preferred_element_type=jnp.float32
    ).reshape(ROPE, prompts, rows)
    rotated = rotate_first(rope_raw, position).astype(jnp.bfloat16).transpose(1, 0, 2)
    moved = []
    for r in range(prompts):
        turn = lambda s: (r + s) % prompts
        send = lax.dynamic_index_in_dim(rotated, turn(z), 0, keepdims=False)
        moved.append(
            lax.ppermute(
                send,
                ("sp", "tp"),
                [
                    (s * n_tp + u, (prompts * u + turn(s)) * n_tp + s // prompts)
                    for s in range(n_sp)
                    for u in range(n_tp)
                ],
            )
        )
    moved = jnp.stack(moved)
    if prompts > 1:
        moved = jnp.concatenate(
            [
                lax.dynamic_index_in_dim(moved, (z - s) % prompts, 0, keepdims=True)
                for s in range(prompts)
            ],
            axis=0,
        )
    ropes = moved[None]
    for b in range(n_tp.bit_length() - 1):
        ropes = jnp.concatenate([ropes, swap(ropes, "tp", 1 << b)], axis=0)
    rope_keys = jnp.concatenate(
        [
            lax.dynamic_index_in_dim(ropes, u ^ t, 0, keepdims=False)[p]
            for u in range(n_tp)
            for p in range(prompts)
        ],
        axis=1,
    )

    table = Table(
        {
            "z": z,
            "x": x,
            "y": y,
            "c": c,
            "prompt_x": (z // per_chip) ^ x,
            "prompt_c": (z // prompts % 2) ^ c,
            "prompt": z % prompts,
        }
    )
    at_c = table.add(c=(0, 1))
    at_half = [table.add(c=(s, half)) for s in range(2)]
    at_keep = [table.add(x=(0, sub), more=p * rows) for p in range(prompts)]
    at_send = [
        table.add(
            prompt_c=(i // prompts % 2, n_x * prompts * sub),
            prompt_x=(i // per_chip, prompts * sub),
            prompt=(i % prompts, sub),
        )
        for i in range(n_sp)
    ]
    at_place = {
        (j, i): table.add(z=(i, rows), x=(j, sub)) for j in range(n_x) for i in range(n_sp)
    }
    at_piece = {(0, 0, 0, 0): table.add(z=(0, k_block))}
    for i, a, j, g in weights:
        at_piece[i, a, j, g] = table.add(
            z=(i, k_block), y=(g, n_x * piece), x=(a ^ j, piece)
        )
    stages = [stage for stage in stages_of(n_sp, n_x, n_grp) if stage]
    numbers = table.build()
    gain = kv_gain[None, :]
    latent = None
    for k, stage in enumerate(stages):
        latent = latent_part(
            numbers,
            (at_c, at_half, at_keep, at_send, at_piece),
            taken,
            w_latent if k == 0 else None,
            [(weights[one], one) for one in stage],
            latent,
            gain if k == len(stages) - 1 else None,
            prompts,
            sub,
            c,
        )
    blocks = {}
    for i in range(n_sp):
        blocks[0, 0, i] = swap(latent[i], "sp", i) if i else latent[0]
        for j in range(1, n_x):
            blocks[0, j, i] = swap(blocks[0, 0, i], "tp", 2 * j)
        for j in range(n_x):
            blocks[1, j, i] = swap(blocks[0, j, i], "tp", 1)
    cut = n_sp // 2
    caches = None
    for low, high in ((0, cut), (cut, n_sp)):
        if low < high:
            caches = final(
                numbers,
                (at_half, at_place),
                {key: block for key, block in blocks.items() if low <= key[2] < high},
                caches,
                (gain, w_up_key, w_up_value, rope_keys, q_nope, q_rope),
                n_sp * rows,
                high == n_sp,
            )
    keys, values, read = caches
    return (keys[None], values[None], rope_keys[None], read)


def fetches(n_sp, n_x):
    if n_sp == 2:
        return [(1, 0)]
    order = [(n_sp - 1, 0), (1, 0)]
    for i in range(2, n_sp - 1):
        order += [(i, a) for a in range(n_x - 1)]
    order += [(1, a) for a in range(1, n_x)]
    return order + [(i, n_x - 1) for i in range(2, n_sp - 1)]


def stages_of(n_sp, n_x, n_grp):
    order = fetches(n_sp, n_x)
    (early, late) = (order[:2], order[2:])
    first = [(i, a, 0, g) for i, a in early for g in range(n_grp)]
    first += [(*one, 0, 0) for one in late[: 1 + n_x]]
    done = set(first)
    rest = [(*one, 0, g) for one in late for g in range(n_grp) if (*one, 0, g) not in done]
    rest += [(*order[0], j, g) for g in range(n_grp) for j in range(1, n_x)]
    return [first, rest]


def latent_part(numbers, at, taken, w_own, pieces, start, gain, prompts, sub, c):
    at_c, at_half, at_keep, at_send, at_piece = at
    n_x = len(taken) // 2
    share = prompts * sub
    own = share * n_x
    kind = taken[0].dtype
    cols = pieces[0][0].shape[1]
    spans = [(at_piece[one], w.shape[0]) for w, one in pieces]
    if w_own is not None:
        spans = [(at_piece[0, 0, 0, 0], w_own.shape[0])] + spans
    depth = sum(size for _, size in spans)
    n_out = len(at_send)
    if any(size % 128 for _, size in spans):
        total = 0.0 if start is None else start
        rows = []
        for q, source in enumerate(taken):
            if q % n_x:
                rows.append(source)
            else:
                rows += [lax.dynamic_slice_in_dim(source, numbers[k], sub, 0) for k in at_keep]
        rows = jnp.concatenate(rows, axis=0)
        picked = [lax.dynamic_slice(rows, (0, numbers[k]), (2 * own, size)) for k, size in spans]
        held = [w for w, _ in pieces]
        if w_own is not None:
            held = [lax.dynamic_slice(w_own, (0, c * cols), (w_own.shape[0], cols))] + held
        total = total + jnp.dot(
            jnp.concatenate(picked, axis=1),
            jnp.concatenate(held, axis=0),
            preferred_element_type=jnp.float32,
        )
        if gain is None:
            return total
        total = (total * lax.dynamic_slice(gain, (0, c * cols), (1, cols))).astype(jnp.bfloat16)
        return [lax.dynamic_slice(total, (numbers[k], 0), (sub, cols)) for k in at_send]

    count = len(pieces)
    n_copies = len(spans) * (2 * (prompts + n_x - 1) + 1) + 1

    def kernel(numbers, *refs):
        refs = list(refs)

        def take(n):
            head = refs[:n]
            del refs[:n]
            return head

        sources = take(len(taken))
        weights = take(count)
        weights_own = take(1) if w_own is not None else None
        first = take(1) if start is not None else None
        scale = take(1) if gain is not None else None
        outs = take(1 if gain is None else n_out)
        rows, weight, *spare, sems = refs
        copies = []

        def copy(source, target):
            copies.append(pltpu.make_async_copy(source, target, sems.at[len(copies)]))

        groups = []
        column = 0
        held = (weights_own or []) + weights
        for q, (k, size) in enumerate(spans):
            before = len(copies)
            place = pl.multiple_of(numbers[k], 128)
            row = 0
            for n, source in enumerate(sources):
                starts = [0] if n % n_x else [pl.multiple_of(numbers[k], 8) for k in at_keep]
                many = share // len(starts)
                for low in starts:
                    copy(
                        source.at[pl.ds(low, many), pl.ds(place, size)],
                        rows.at[pl.ds(row, many), pl.ds(column, size)],
                    )
                    row += many
            source = held[q]
            if q == 0 and weights_own is not None:
                source = source.at[:, pl.ds(pl.multiple_of(numbers[at_half[0]], 128), cols)]
            copy(source, weight.at[pl.ds(column, size)])
            new = copies[before:]
            if groups and groups[-1][1] - groups[-1][0] + size <= 1024:
                groups[-1] = (groups[-1][0], column + size, groups[-1][2] + new)
            else:
                groups.append((column, column + size, new))
            column += size
        if first is not None:
            copy(first[0], spare[-1])
        for one in copies:
            one.start()
        total = None
        for low, high, some in groups:
            for one in some:
                one.wait()
            part = jnp.dot(
                rows[:, low:high], weight[low:high, :], preferred_element_type=jnp.float32
            )
            total = part if total is None else total + part
        if first is not None:
            copies[-1].wait()
            total = total + spare[-1][...]
        if scale is None:
            outs[0][...] = total
        else:
            side = numbers[at_c] == 0
            here = jnp.where(side, scale[0][:, :cols], scale[0][:, cols:])
            spare[0][...] = (total * here).astype(jnp.bfloat16)
            for i in range(n_out):
                outs[i][...] = spare[0][pl.ds(pl.multiple_of(numbers[at_send[i]], sub), sub), :]

    whole = pl.BlockSpec(memory_space=pltpu.VMEM)
    smem = pl.BlockSpec(memory_space=pltpu.SMEM)
    hbm = pl.BlockSpec(memory_space=pl.ANY)
    operands = list(taken) + [w for w, _ in pieces] + ([w_own] if w_own is not None else [])
    kinds = [hbm] * len(operands) + ([hbm] if start is not None else [])
    kinds += [whole] if gain is not None else []
    extra = ([start] if start is not None else []) + ([gain] if gain is not None else [])
    if gain is None:
        out = (jax.ShapeDtypeStruct((2 * own, cols), jnp.float32),)
        spare = []
    else:
        out = (jax.ShapeDtypeStruct((sub, cols), jnp.bfloat16),) * n_out
        spare = [pltpu.VMEM((2 * own, cols), jnp.bfloat16)]
    if start is not None:
        spare = spare + [pltpu.VMEM((2 * own, cols), jnp.float32)]
    result = pl.pallas_call(
        kernel,
        out_shape=out,
        in_specs=[smem] + kinds,
        out_specs=(whole,) * len(out),
        scratch_shapes=[pltpu.VMEM((2 * own, depth), kind), pltpu.VMEM((depth, cols), kind)]
        + spare
        + [pltpu.SemaphoreType.DMA((n_copies,))],
        cost_estimate=pl.CostEstimate(
            flops=4 * own * cols * depth, bytes_accessed=4 * own * depth, transcendentals=0
        ),
    )(numbers, *operands, *extra)
    return result[0] if gain is None else result


def final(numbers, at, blocks, caches, others, length, last):
    at_half, at_place = at
    gain, w_up_key, w_up_value, rope_keys, q_nope, q_rope = others
    rank, head_cols = w_up_key.shape
    heads = head_cols // HEAD
    cols = rank // 2
    sub = next(iter(blocks.values())).shape[0]
    here = sorted({key[1:] for key in blocks})
    before = [key for key in sorted(at_place) if key not in here] if caches is not None else []
    n_rows = len(here) * sub
    names = sorted(blocks)

    def kernel(numbers, *refs):
        refs = list(refs)

        def take(n):
            head = refs[:n]
            del refs[:n]
            return head

        gain, up_key, up_value = take(3)
        rope, query, rotary = take(3) if last else (None, None, None)
        pieces = dict(zip(names, take(len(names))))
        old = take(2) if caches is not None else None
        out_k, out_v = take(2)
        read = take(1)[0] if last else None
        latent, wk, wv, keys, values, sems = refs
        copies = []

        def copy(source, target):
            one = pltpu.make_async_copy(source, target, sems.at[len(copies)])
            copies.append(one)
            one.start()
            return one

        loads = []
        for k, key in enumerate(here):
            for s in range(2):
                loads.append(
                    copy(
                        pieces[(s, *key)],
                        latent.at[
                            pl.ds(k * sub, sub),
                            pl.ds(pl.multiple_of(numbers[at_half[s]], 128), cols),
                        ],
                    )
                )
        load_k = copy(up_key, wk)
        load_v = copy(up_value, wv)
        known = []
        if last:
            for key in before:
                place = pl.ds(pl.multiple_of(numbers[at_place[key]], sub), sub)
                known.append(copy(out_k.at[place], keys.at[place]))
                known.append(copy(out_v.at[place], values.at[place]))
        inverse = 1.0 / gain[...]
        for one in loads:
            one.wait()
        stores = []
        factors = []
        for weight, load, cache, out in (
            (wk, load_k, keys, out_k),
            (wv, load_v, values, out_v),
        ):
            load.wait()
            for k in range(0, len(here), 2):
                group = here[k : k + 2]
                rows = latent[k * sub : (k + len(group)) * sub, :]
                if load is load_k:
                    plain = rows.astype(jnp.float32) * inverse
                    squares = jnp.sum(plain * plain, axis=1, keepdims=True)
                    factors.append(lax.rsqrt(squares / rank + EPS))
                got = jnp.dot(rows, weight[...], preferred_element_type=jnp.float32)
                got = (got * factors[k // 2]).astype(cache.dtype)
                for q, key in enumerate(group):
                    place = pl.ds(pl.multiple_of(numbers[at_place[key]], sub), sub)
                    cache[place, :] = got[q * sub : (q + 1) * sub, :]
                    stores.append(copy(cache.at[place], out.at[place]))
        if last:
            for one in known:
                one.wait()

            def apart(flat, width):
                head = lax.broadcasted_iota(jnp.int32, (heads, heads * width), 0)
                column = lax.broadcasted_iota(jnp.int32, (heads, heads * width), 1)
                return jnp.where(column // width == head, flat.astype(jnp.float32), 0.0)

            fold = lax.broadcasted_iota(jnp.int32, (heads * ROPE, ROPE), 0) % ROPE
            fold = fold == lax.broadcasted_iota(jnp.int32, (heads * ROPE, ROPE), 1)
            turned = jnp.dot(
                apart(rotary[...], ROPE).astype(jnp.bfloat16),
                fold.astype(jnp.float32).astype(jnp.bfloat16),
                preferred_element_type=jnp.float32,
            ).astype(jnp.bfloat16)
            scores = lax.dot_general(
                apart(query[...], HEAD).astype(jnp.bfloat16),
                keys[...],
                (((1,), (1,)), ((), ())),
                preferred_element_type=jnp.float32,
            )
            scores = scores + jnp.dot(turned, rope[...], preferred_element_type=jnp.float32)
            scores = scores / jnp.sqrt(jnp.float32(HEAD + ROPE))
            expo = jnp.exp(scores - jnp.max(scores, axis=-1, keepdims=True))
            weights = (expo / jnp.sum(expo, axis=-1, keepdims=True)).astype(jnp.bfloat16)
            mixed = jnp.dot(weights, values[...], preferred_element_type=jnp.float32)
            head = lax.broadcasted_iota(jnp.int32, (heads, head_cols), 0)
            column = lax.broadcasted_iota(jnp.int32, (heads, head_cols), 1)
            mixed = jnp.where(column // HEAD == head, mixed, 0.0)
            read[...] = jnp.sum(mixed, axis=0, keepdims=True).astype(read.dtype)
        for one in stores:
            one.wait()

    whole = pl.BlockSpec(memory_space=pltpu.VMEM)
    smem = pl.BlockSpec(memory_space=pltpu.SMEM)
    hbm = pl.BlockSpec(memory_space=pl.ANY)
    cache = jax.ShapeDtypeStruct((length, head_cols), jnp.bfloat16)
    out = [cache, cache]
    specs = [hbm, hbm]
    operands = [gain, w_up_key, w_up_value]
    kinds = [whole, hbm, hbm]
    if last:
        out.append(jax.ShapeDtypeStruct((1, head_cols), jnp.bfloat16))
        specs.append(whole)
        operands += [rope_keys, q_nope, q_rope]
        kinds += [whole] * 3
    operands += [blocks[name] for name in names]
    kinds += [hbm] * len(names)
    aliases = {}
    if caches is not None:
        aliases = {1 + len(operands): 0, 2 + len(operands): 1}
        operands += list(caches[:2])
        kinds += [hbm, hbm]
    return pl.pallas_call(
        kernel,
        out_shape=tuple(out),
        in_specs=[smem] + kinds,
        out_specs=tuple(specs),
        input_output_aliases=aliases,
        scratch_shapes=[
            pltpu.VMEM((n_rows, rank), jnp.bfloat16),
            pltpu.VMEM((rank, head_cols), w_up_key.dtype),
            pltpu.VMEM((rank, head_cols), w_up_key.dtype),
            pltpu.VMEM((length, head_cols), jnp.bfloat16),
            pltpu.VMEM((length, head_cols), jnp.bfloat16),
            pltpu.SemaphoreType.DMA((4 * len(here) + 2 * len(before) + 2,)),
        ],
        cost_estimate=pl.CostEstimate(
            flops=4 * n_rows * rank * head_cols, bytes_accessed=8 * rank * head_cols, transcendentals=0
        ),
    )(numbers, *operands)


def gathered(
    tokens, offsets, in_gain, w_latent, w_rope_key, kv_gain, w_up_key, w_up_value, q_nope, q_rope
):
    prompts, rows, width = tokens.shape
    n_sp = lax.axis_size("sp")
    length = n_sp * rows
    block = lax.axis_index("sp")
    normed = rms_scale(tokens.reshape(prompts * rows, width), in_gain).astype(jnp.bfloat16)
    latent_raw = jnp.dot(
        normed,
        lax.all_gather(w_latent, "sp", axis=0, tiled=True),
        preferred_element_type=jnp.float32,
    )
    latent = rms_scale(latent_raw, kv_gain).astype(jnp.bfloat16)
    position = offsets[:, None] + block * rows + jnp.arange(rows, dtype=jnp.int32)[None, :]
    rope_raw = jnp.dot(normed, w_rope_key, preferred_element_type=jnp.float32).reshape(
        prompts, rows, ROPE
    )
    rotated = rotate(rope_raw, position).astype(jnp.bfloat16)
    latent_every, rope_every = (
        lax.all_gather(latent.reshape(prompts, rows, latent.shape[1]), "tp", axis=0, tiled=True),
        lax.all_gather(rotated, "tp", axis=0, tiled=True),
    )
    latent_moved, rope_moved = (
        lax.all_to_all(latent_every[:, None], "sp", split_axis=0, concat_axis=1, tiled=True),
        lax.all_to_all(rope_every[:, None], "sp", split_axis=0, concat_axis=1, tiled=True),
    )
    latent_all = latent_moved.reshape(length, latent_moved.shape[3])
    keys = jnp.dot(latent_all, w_up_key, preferred_element_type=jnp.float32).astype(jnp.bfloat16)
    values = jnp.dot(latent_all, w_up_value, preferred_element_type=jnp.float32).astype(
        jnp.bfloat16
    )
    rope_keys = rope_moved.reshape(length, ROPE).T
    read = attend(keys, values, rope_keys, q_nope, q_rope)
    return (keys[None], values[None], rope_keys[None], read)


def local(tokens, *rest):
    prompts, rows, _ = tokens.shape
    n_sp, n_tp, n_grp = (lax.axis_size("sp"), lax.axis_size("tp"), lax.axis_size("grp"))
    w_latent = rest[2]
    twos = all(n & (n - 1) == 0 for n in (n_sp, n_tp, n_grp))
    if (
        twos
        and n_tp > 1
        and n_sp == prompts * n_tp
        and rows % (n_tp // 2) == 0
        and w_latent.shape[0] % (n_tp // 2 * n_grp * 2) == 0
        and w_latent.shape[1] % 2 == 0
    ):
        return spread(tokens, *rest)
    return gathered(tokens, *rest)


def solution(mesh):
    in_specs = (
        P(("grp", "tp"), "sp", None),
        P(("grp", "tp")),
        P(),
        P("sp", None),
        P(),
        P(),
        P(None, "tp"),
        P(None, "tp"),
        P(("grp", "sp"), "tp"),
        P(("grp", "sp"), "tp"),
    )
    out_specs = (
        P(("grp", "sp"), None, "tp"),
        P(("grp", "sp"), None, "tp"),
        P(("grp", "sp"), None, None),
        P(("grp", "sp"), "tp"),
    )

    return jax.shard_map(local, mesh=mesh, in_specs=in_specs, out_specs=out_specs, check_vma=False)
```
